256 devices in a mesh: grp: 2 (over y), sp: 16 (over z), tp: 8 (over x, core).
Axes of the slice: x: 4, y: 2, z: 16, core: 2. Of those that a mesh axis runs over, the one named last changes fastest.
The devices are a block of a 4x16x16 slice.
Arguments:
- tokens: bfloat16 [32768, 2048], P(('grp', 'sp')), parts along dimension 0, may hold values from -6 to 6
- doc_ids: int32 [32768], P(('grp', 'sp')), parts along dimension 0, may hold values from 0 to 3, never falling along the last dimension, each value on 1 to 8192 neighbouring positions
- gains: bfloat16 [2, 2048], replicated, may hold values from 0.099609375 to 1.8984375
- w_query: bfloat16 [2, 2048, 1024], P(None, None, 'tp'), may hold values from -0.125 to 0.125
- w_key: bfloat16 [2, 2048, 1024], P(None, None, 'tp'), may hold values from -0.125 to 0.125
- w_value: bfloat16 [2, 2048, 1024], P(None, None, 'tp'), may hold values from -0.125 to 0.125
- rel_table: float32 [2, 16, 257], P(None, 'tp'), may hold values from -6 to 270
- out_first: bfloat16 [1024, 2048], replicated, may hold values from -0.5 to 0.5
- out_last: bfloat16 [1024, 2048], P(None, 'tp'), may hold values from -0.5 to 0.5
Outputs:
- mixed: bfloat16 [32768, 2048], P(('grp', 'sp'), 'tp'), parts along dimension 0
The draws below stay inside these ranges and needn't reach their ends.
There are 2 independent parts, one for each index of `grp`. The reference program is written for one: setup_inputs(seed, part) draws one part's arguments, and reference() takes and returns one part's arrays. A program takes and returns all parts, laid end to end along the dimension named above; an argument that names none is the same for every part. Nothing has to cross between parts.
Inputs may be any that keep to these rules, and one draw needn't show every extreme that they name: `doc_ids`: document numbers never fall along the sequence.
All inputs are finite; a program needn't handle non-finite values.
Results may differ from the reference program's by a relative error of at most 0.014.
Values may be sent and summed in bfloat16 or wider, within the bound.
A program may use at most 128 MiB of HBM per device.

```python
import math
import jax
import jax.numpy as jnp
import numpy as np
from jax import lax

D = 2048
HEADS = 16
HEAD_DIM = 64
SEG = 64
PREV_SEGS = 8
MAX_REL = 128
LAYERS = 2
TOKENS = 16384
DOCS = 4


def draw_rel_table(key, part):
    shape = (LAYERS, HEADS, 2 * MAX_REL + 1)
    return jnp.clip(jax.random.normal(key, shape, jnp.float32), -4.0, 4.0)


def shard_levels(stream_key, dims, shards, smallest, largest):
    def one(position, parts):
        heights = jax.random.uniform(jax.random.fold_in(jax.random.fold_in(stream_key, 6), position), (parts,), jnp.float32, smallest / len(shards), largest / len(shards))
        return jnp.repeat(jnp.exp(heights), dims[position] // parts).reshape((-1,) + (1,) * (len(dims) - position - 1))

    factor_of = one(*shards[0])
    for cut in shards[1:]:
        factor_of = factor_of * one(*cut)
    return factor_of


def profile(count, total, limit, skew):
    weights = [(1 << 20) // math.isqrt(rank ** skew) + 1 for rank in range(2, count + 1)]
    surplus, counts = total - limit - (count - 1), [1] * (count - 1)
    while surplus > 0:
        movable = [i for i in range(count - 1) if counts[i] < limit]
        whole, remaining = sum([weights[i] for i in movable]), surplus
        for i in movable:
            addition = min(limit - counts[i], max(1, remaining * weights[i] // whole), surplus)
            counts[i] = counts[i] + addition
            surplus = surplus - addition
    return np.array([limit] + counts)


def ragged_sizes(stream_key, count, total, limit, lean):
    if count == 2:
        one = jax.random.randint(stream_key, (), max(1, total - limit), min(limit, total - 1) + 1)
        return jnp.stack([one, total - one])
    tallies = jnp.asarray(profile(count, total, limit, lean), jnp.int32)
    pairs = (count - 1) // 2
    source_of, taker = tallies[1:1 + 2 * pairs:2], tallies[2:2 + 2 * pairs:2]
    room = jnp.minimum(source_of - 1, limit - taker)
    passed = jax.random.randint(jax.random.fold_in(stream_key, 1), (pairs,), 0, 1 << 20) % (room + 1)
    tallies = tallies.at[1:1 + 2 * pairs:2].set(source_of - passed).at[2:2 + 2 * pairs:2].set(taker + passed)
    return tallies[jax.random.permutation(jax.random.fold_in(stream_key, 2), count)]


def gaussian(rng, shape, scale, most, pieces=(), kind=jnp.bfloat16):
    array = scale * jax.random.normal(rng, shape, jnp.float32)
    if pieces:
        array = array * shard_levels(rng, shape, pieces, -0.22, 0.18)
    return jnp.clip(array, -most, most).astype(kind)


def setup_inputs(seed: int = 0, part: int = 0) -> dict:
    splits = jax.random.split(jax.random.key(seed), 10)
    part_splits = jax.random.split(jax.random.fold_in(splits[9], part), 10)
    tokens = gaussian(part_splits[0], (TOKENS, D), 1.0, 6.0, ((0, 16),))
    doc_ids = jnp.searchsorted(jnp.cumsum(ragged_sizes(part_splits[1], DOCS, TOKENS, TOKENS // 2, 1)), jnp.arange(TOKENS), side="right").astype(jnp.int32)
    gains = jnp.clip(1.0 + 0.18 * jax.random.normal(splits[2], (LAYERS, D), jnp.float32), 0.099609375, 1.8984375).astype(jnp.bfloat16)
    w_query = gaussian(splits[3], (LAYERS, D, HEADS * HEAD_DIM), D ** -0.5, 0.125, ((2, 8),))
    w_key = gaussian(splits[4], (LAYERS, D, HEADS * HEAD_DIM), D ** -0.5, 0.125, ((2, 8),))
    w_value = gaussian(splits[5], (LAYERS, D, HEADS * HEAD_DIM), D ** -0.5, 0.125, ((2, 8),))
    rel_table = draw_rel_table(jax.random.fold_in(splits[9], 71), part)
    out_first = gaussian(splits[7], (HEADS * HEAD_DIM, D), (HEADS * HEAD_DIM // 9) ** -0.5, 0.5)
    out_last = gaussian(splits[8], (HEADS * HEAD_DIM, D), (HEADS * HEAD_DIM // 9) ** -0.5, 0.5, ((1, 8),))
    return {"tokens": tokens, "doc_ids": doc_ids, "gains": gains, "w_query": w_query, "w_key": w_key, "w_value": w_value, "rel_table": rel_table, "out_first": out_first, "out_last": out_last}


def normalize(stream, gain_row):
    values32 = stream.astype(jnp.float32)
    scaled = values32 * lax.rsqrt(lax.optimization_barrier(jnp.mean(values32 * values32, axis=-1, keepdims=True)) + 1e-06)
    return (scaled * gain_row.astype(jnp.float32)).astype(jnp.bfloat16)

def banded(key_rows, seg_count):
    by_segment = key_rows.reshape((seg_count + PREV_SEGS, SEG) + key_rows.shape[1:])
    stacked = jnp.stack([by_segment[offset_seg:offset_seg + seg_count] for offset_seg in range(PREV_SEGS + 1)], axis=1)
    return stacked.reshape((seg_count, (PREV_SEGS + 1) * SEG) + key_rows.shape[1:])

def attend(queries, pad_keys, pad_values, query_docs, pad_docs, bias_table):
    seq_rows = queries.shape[0]
    seg_count = seq_rows // SEG
    head_count = bias_table.shape[0]
    head_width = queries.shape[1] // head_count
    band_rows = (PREV_SEGS + 1) * SEG
    query_blocks = queries.reshape(seg_count, SEG, head_count, head_width).astype(jnp.float32)
    key_band = banded(pad_keys.reshape(-1, head_count, head_width), seg_count).astype(jnp.float32)
    value_band = banded(pad_values.reshape(-1, head_count, head_width), seg_count).astype(jnp.float32)
    query_pos = jnp.arange(SEG, dtype=jnp.int32)[:, None]
    band_pos = jnp.arange(band_rows, dtype=jnp.int32)[None, :]
    rel_index = jnp.clip(PREV_SEGS * SEG + query_pos - band_pos, -MAX_REL, MAX_REL) + MAX_REL
    bias = jnp.take(bias_table.astype(jnp.float32), rel_index, axis=1)
    scores = jnp.einsum('nqhd,nkhd->nhqk', query_blocks, key_band) * head_width ** (-0.5) + bias[None]
    doc_band = banded(pad_docs, seg_count)
    allowed = doc_band[:, None, None, :] == query_docs.reshape(seg_count, 1, SEG, 1)
    scores = jnp.where(allowed, scores, jnp.float32(-1e+30))
    row_max = lax.optimization_barrier(jnp.max(scores, axis=-1, keepdims=True))
    exp_scores = jnp.exp(scores - row_max)
    probs = exp_scores / lax.optimization_barrier(jnp.sum(exp_scores, axis=-1, keepdims=True))
    weights = probs.astype(jnp.bfloat16).astype(jnp.float32)
    result = jnp.einsum('nhqk,nkhd->nqhd', weights, value_band)
    return result.astype(jnp.bfloat16).reshape(seq_rows, head_count * head_width)

def reference(tokens, doc_ids, gains, w_query, w_key, w_value, rel_table, out_first, out_last):
    reach_rows = PREV_SEGS * SEG
    pad_docs = jnp.concatenate([jnp.full((reach_rows,), -1, jnp.int32), doc_ids.astype(jnp.int32)])
    hidden = tokens
    for layer_number in range(LAYERS):
        normed = normalize(hidden, gains[layer_number])
        queries = jnp.dot(normed, w_query[layer_number], preferred_element_type=jnp.float32).astype(jnp.bfloat16)
        keys = jnp.dot(normed, w_key[layer_number], preferred_element_type=jnp.float32).astype(jnp.bfloat16)
        values = jnp.dot(normed, w_value[layer_number], preferred_element_type=jnp.float32).astype(jnp.bfloat16)
        blank = jnp.zeros((reach_rows, keys.shape[1]), jnp.bfloat16)
        attended = attend(queries, jnp.concatenate([blank, keys]), jnp.concatenate([blank, values]), doc_ids, pad_docs, rel_table[layer_number])
        weight = out_first if layer_number == 0 else out_last
        update = jnp.dot(attended, weight, preferred_element_type=jnp.float32)
        hidden = (hidden.astype(jnp.float32) + update).astype(jnp.bfloat16)
    return hidden
```

```python
import functools
import math

import jax
import jax.numpy as jnp
from jax import lax
from jax.experimental import pallas as pl
from jax.experimental.pallas import tpu as pltpu
from jax.sharding import PartitionSpec as P

SEG = 64
PREV_SEGS = 8
MAX_REL = 128
LAYERS = 2
HEAD_DIM = 64
REACH = SEG * PREV_SEGS
PAIR = 2 * SEG
WIN = REACH + PAIR
CHUNK = 2 * PAIR
BIG = 1e30
LOG2E = math.log2(math.e)
MESH = pl.DeviceIdType.MESH
BF = jnp.bfloat16
F32 = jnp.float32


def kernel(
    sp_n,
    tp_n,
    tokens,
    docs,
    gains,
    w_query,
    w_key,
    w_value,
    table,
    out_first,
    out_last,
    mixed,
    h,
    lhs,
    wqkv,
    wfirst,
    wlast,
    qbuf,
    qext,
    kbuf,
    kext,
    vt,
    att,
    bias,
    halo_docs,
    res,
    load_sem,
    store_sem,
    halo_send,
    halo_recv,
    ag_send,
    ag_recv,
):
    rows, width = h.shape
    cols = wlast.shape[1]
    pairs = rows // PAIR
    chunks = rows // CHUNK
    tail = REACH // CHUNK
    sp = lax.axis_index("sp")
    me = lax.axis_index("tp")
    succ = {"sp": lax.rem(sp + 1, sp_n)}
    pred = {"sp": lax.rem(sp + sp_n - 1, sp_n)}
    left_i = lax.rem(me + tp_n - 2, tp_n)
    right_i = lax.rem(me + 2, tp_n)
    far_i = lax.rem(me + 4, tp_n)
    partner_i = me + 1 - 2 * lax.rem(me, 2)
    left, right, partner = {"tp": left_i}, {"tp": right_i}, {"tp": partner_i}
    order = list(range(chunks))[::-1]

    barrier = pltpu.get_barrier_semaphore()
    for other in (left, right, partner, succ, pred):
        pl.semaphore_signal(barrier, inc=1, device_id=other, device_id_type=MESH)

    loads = {}

    def load(name, src, dst):
        copy = pltpu.make_async_copy(src, dst, load_sem.at[len(loads)])
        copy.start()
        loads[name] = copy

    def load_w(layer):
        for i, w in enumerate((w_query, w_key, w_value)):
            load(("w", layer, i), w.at[layer], wqkv.at[layer, :, pl.ds(i * 128, 128)])

    def chunk_rows(c):
        return pl.ds(c * CHUNK, CHUNK)

    load(("t", order[0]), tokens.at[chunk_rows(order[0])], h.at[chunk_rows(order[0])])
    load_w(0)
    for c in order[1:]:
        load(("t", c), tokens.at[chunk_rows(c)], h.at[chunk_rows(c)])
    load("first", out_first, wfirst)
    load_w(1)
    load("last", out_last, wlast)

    lane = lax.broadcasted_iota(jnp.int32, (PAIR, 128), 1)
    lane_f = lane.astype(F32)

    def doc_columns(row):
        return jnp.broadcast_to(row.astype(F32), (128, 128)).T

    def build_docs():
        for b in range(rows // 128):
            col = doc_columns(docs[b : b + 1, :])
            same = col == lane_f
            kext[pl.ds(REACH + 128 * b, 128), :] = jnp.where(same, 1.0, 0.0).astype(BF)
            qext[pl.ds(128 * b, 128), :] = jnp.where(same, 0.0, -BIG).astype(BF)

    def build_halo_docs():
        void = jnp.where(sp == 0, 1.0, 0.0).astype(F32)
        for b in range(REACH // 128):
            r = (rows - REACH) // 128 + b
            col = doc_columns(halo_docs[r : r + 1, :])
            one_hot = jnp.where(col == lane_f, 1.0, 0.0)
            kext[pl.ds(128 * b, 128), :] = jnp.where(lane == 127, void, one_hot).astype(BF)

    def build_bias(layer):
        row = lax.broadcasted_iota(jnp.int32, (PAIR, PAIR), 0)
        col = lax.broadcasted_iota(jnp.int32, (PAIR, PAIR), 1)
        for n in range(2):
            near = table[layer, n : n + 1, 0 : 2 * MAX_REL]
            edge = table[layer, n : n + 1, 2 * MAX_REL : 2 * MAX_REL + 1]
            near = (near - edge) * LOG2E
            upper = jnp.concatenate([near[:, 128:], jnp.zeros((1, 128), F32)], axis=1)
            for part, values in ((0, upper), (1, near)):
                turned = pltpu.roll(
                    jnp.broadcast_to(values, (128, 256)), 128, 1, stride=1, stride_axis=0
                )[:, :128]
                if part == 1:
                    turned = jnp.where((row >= SEG) & (col < SEG), -BIG, turned)
                bias[layer, pl.ds(128 * part, 128), pl.ds(128 * n, 128)] = turned

    def project_qkv(layer, c, square_sum):
        scale = lax.rsqrt(square_sum * (1.0 / width) + 1e-06)
        qkv = jnp.dot(lhs[...], wqkv[layer], preferred_element_type=F32)
        q = qkv[:, 0:128] * (scale * (HEAD_DIM**-0.5 * LOG2E))
        k = qkv[:, 128:256] * scale
        v = qkv[:, 256:384] * scale
        wide = lax.broadcasted_iota(jnp.int32, (CHUNK, 128), 1)
        qbuf[0, chunk_rows(c), :] = jnp.where(wide < HEAD_DIM, q, 0.0).astype(BF)
        qbuf[1, chunk_rows(c), :] = jnp.where(wide < HEAD_DIM, 0.0, q).astype(BF)
        kbuf[layer, pl.ds(REACH + CHUNK * c, CHUNK), :] = k.astype(BF)
        for i in range(2):
            block = v[128 * i : 128 * (i + 1), :].T
            vt[layer, REACH // 128 + 2 * c + i] = block.astype(BF)

    def gain_row(layer, n, step):
        return gains[layer : layer + 1, pl.ds(n * step, step)].astype(F32)

    def dense(c):
        step = 256
        total = jnp.zeros((CHUNK, 128), F32)
        for n in range(width // step):
            x = h[chunk_rows(c), pl.ds(n * step, step)].astype(F32)
            square = x * x
            for j in range(step // 128):
                total = total + square[:, 128 * j : 128 * (j + 1)]
            lhs[:, pl.ds(n * step, step)] = (x * gain_row(0, n, step)).astype(BF)
        project_qkv(0, c, jnp.sum(total, axis=1, keepdims=True))

    def attended_rows(layer, c):
        return jnp.concatenate([att[layer, t, chunk_rows(c), :] for t in range(tp_n)], axis=1)

    def trans(c):
        step = 256
        a = attended_rows(0, c)
        total = jnp.zeros((CHUNK, 128), F32)
        for n in range(width // step):
            part = pl.ds(n * step, step)
            update = jnp.dot(a, wfirst[:, part], preferred_element_type=F32)
            x = (h[chunk_rows(c), part].astype(F32) + update).astype(BF)
            h[chunk_rows(c), part] = x
            x = x.astype(F32)
            square = x * x
            for j in range(step // 128):
                total = total + square[:, 128 * j : 128 * (j + 1)]
            lhs[:, part] = (x * gain_row(1, n, step)).astype(BF)
        project_qkv(1, c, jnp.sum(total, axis=1, keepdims=True))

    def final(c):
        a = attended_rows(1, c)
        update = jnp.dot(a, wlast[...], preferred_element_type=F32)
        own = h[chunk_rows(c), pl.ds(pl.multiple_of(me * cols, cols), cols)].astype(F32)
        res[chunk_rows(c), :] = (own + update).astype(BF)
        copy = pltpu.make_async_copy(
            res.at[chunk_rows(c)], mixed.at[chunk_rows(c)], store_sem.at[c]
        )
        copy.start()
        return copy

    def attend(layer, p):
        window = pl.ds(PAIR * p, WIN)
        mine = pl.ds(PAIR * p, PAIR)
        keys = jnp.concatenate([kbuf[layer, window, :], kext[window, :]], axis=1)
        queries = jnp.concatenate(
            [
                jnp.concatenate([qbuf[0, mine, :], qext[mine, :]], axis=1),
                jnp.concatenate([qbuf[1, mine, :], qext[mine, :]], axis=1),
            ],
            axis=0,
        )
        s = lax.dot_general(
            keys, queries, (((1,), (1,)), ((), ())), preferred_element_type=F32
        )
        first = lax.broadcasted_iota(jnp.int32, (SEG, 2 * PAIR), 1)
        s_first = jnp.where(lax.rem(first, PAIR) < SEG, s[:SEG], -BIG)
        s = jnp.concatenate([s_first, s[SEG : WIN - 256], s[WIN - 256 :] + bias[layer]], axis=0)
        e = jnp.exp2(s - jnp.max(s, axis=0, keepdims=True))
        inverse = 1.0 / jnp.sum(e, axis=0, keepdims=True)
        values = jnp.concatenate([vt[layer, p + i] for i in range(WIN // 128)], axis=1)
        o = jnp.dot(values, e.astype(BF), preferred_element_type=F32)
        o = jnp.concatenate(
            [
                o[:HEAD_DIM, :PAIR] * inverse[:, :PAIR],
                o[HEAD_DIM:, PAIR:] * inverse[:, PAIR:],
            ],
            axis=0,
        )
        att[layer, me, mine, :] = o.T.astype(BF)

    sent = []

    def remote(src, dst, send_sem, recv_sem, device):
        return pltpu.make_async_remote_copy(
            src_ref=src,
            dst_ref=dst,
            send_sem=send_sem,
            recv_sem=recv_sem,
            device_id=device,
            device_id_type=MESH,
        )

    def start(copy):
        copy.start()
        sent.append(copy)

    def halo(layer, c):
        i = layer * tail + c - (chunks - tail)
        k0 = CHUNK * (c - (chunks - tail))
        b0 = k0 // 128
        return (
            remote(
                kbuf.at[layer, pl.ds(REACH + CHUNK * c, CHUNK)],
                kbuf.at[layer, pl.ds(k0, CHUNK)],
                halo_send.at[2 * i],
                halo_recv.at[2 * i],
                succ,
            ),
            remote(
                vt.at[layer, pl.ds(REACH // 128 + 2 * c, 2)],
                vt.at[layer, pl.ds(b0, 2)],
                halo_send.at[2 * i + 1],
                halo_recv.at[2 * i + 1],
                succ,
            ),
        )

    def doc_halo():
        i = 2 * LAYERS * tail
        return remote(docs, halo_docs, halo_send.at[i], halo_recv.at[i], succ)

    def send_halo(layer, c):
        for copy in halo(layer, c):
            start(copy)

    def wait_halo(layer, c):
        for copy in halo(layer, c):
            copy.wait_recv()

    def block(layer, p, kind, slot, device, part=None):
        first = PAIR * p + (SEG if part == 1 else 0)
        ref = att.at[layer, slot, pl.ds(first, PAIR if part is None else SEG)]
        i = (layer * pairs + p) * 8 + kind
        return remote(ref, ref, ag_send.at[i], ag_recv.at[i], device)

    def send_own(layer, p):
        start(block(layer, p, 0, me, right))
        start(block(layer, p, 1, me, left))
        start(block(layer, p, 2, me, partner))

    def relay1(layer, p):
        block(layer, p, 0, left_i, right).wait_recv()
        start(block(layer, p, 3, left_i, right, 0))
        start(block(layer, p, 4, left_i, partner))
        block(layer, p, 1, right_i, left).wait_recv()
        start(block(layer, p, 5, right_i, left, 1))
        start(block(layer, p, 6, right_i, partner))

    def relay2(layer, p):
        block(layer, p, 3, far_i, right, 0).wait_recv()
        block(layer, p, 5, far_i, left, 1).wait_recv()
        start(block(layer, p, 7, far_i, partner))

    def consume(layer, p):
        block(layer, p, 2, partner_i, partner).wait_recv()
        block(layer, p, 4, lax.rem(partner_i + tp_n - 2, tp_n), partner).wait_recv()
        block(layer, p, 6, lax.rem(partner_i + 2, tp_n), partner).wait_recv()
        block(layer, p, 7, lax.rem(partner_i + 4, tp_n), partner).wait_recv()

    def attend_send(layer, *which):
        for p in which:
            attend(layer, p)
            send_own(layer, p)

    build_docs()
    for layer in range(LAYERS):
        build_bias(layer)
    for i in range(3):
        loads[("w", 0, i)].wait()
    c3, c2, c1, c0 = order
    loads[("t", c3)].wait()
    dense(c3)
    pl.semaphore_wait(barrier, 5)
    start(doc_halo())
    send_halo(0, c3)
    loads[("t", c2)].wait()
    dense(c2)
    send_halo(0, c2)
    loads[("t", c1)].wait()
    dense(c1)
    attend_send(0, 7, 6)
    loads[("t", c0)].wait()
    dense(c0)
    attend_send(0, 5, 4)
    doc_halo().wait_recv()
    build_halo_docs()
    wait_halo(0, c3)
    attend_send(0, 3, 2)
    relay1(0, 7)
    relay1(0, 6)
    wait_halo(0, c2)
    attend_send(0, 1, 0)
    relay1(0, 5)
    relay2(0, 7)
    relay1(0, 4)
    relay2(0, 6)
    relay1(0, 3)
    loads["first"].wait()
    for i in range(3):
        loads[("w", 1, i)].wait()
    loads["last"].wait()
    consume(0, 7)
    consume(0, 6)
    trans(c3)
    send_halo(1, c3)
    relay2(0, 5)
    relay1(0, 2)
    relay2(0, 4)
    relay1(0, 1)
    relay1(0, 0)
    consume(0, 5)
    consume(0, 4)
    trans(c2)
    send_halo(1, c2)
    relay2(0, 3)
    relay2(0, 2)
    relay2(0, 1)
    relay2(0, 0)
    consume(0, 3)
    consume(0, 2)
    trans(c1)
    attend_send(1, 7, 6)
    consume(0, 1)
    consume(0, 0)
    trans(c0)
    relay1(1, 7)
    attend_send(1, 5, 4)
    relay1(1, 6)
    wait_halo(1, c3)
    attend_send(1, 3, 2)
    relay1(1, 5)
    relay2(1, 7)
    wait_halo(1, c2)
    attend_send(1, 1, 0)
    relay1(1, 4)
    relay2(1, 6)
    relay1(1, 3)
    relay2(1, 5)
    consume(1, 7)
    consume(1, 6)
    stores = [final(c3)]
    relay1(1, 2)
    relay2(1, 4)
    relay1(1, 1)
    relay2(1, 3)
    relay1(1, 0)
    consume(1, 5)
    consume(1, 4)
    stores.append(final(c2))
    relay2(1, 2)
    relay2(1, 1)
    relay2(1, 0)
    consume(1, 3)
    consume(1, 2)
    stores.append(final(c1))
    consume(1, 1)
    consume(1, 0)
    stores.append(final(c0))
    for copy in sent:
        copy.wait_send()
    for copy in stores:
        copy.wait()


def solution(mesh):
    sp_n, tp_n = mesh.shape["sp"], mesh.shape["tp"]

    def shards(tokens, doc_ids, gains, w_query, w_key, w_value, rel_table, out_first, out_last):
        rows, width = tokens.shape
        cols = out_last.shape[1]
        depth = out_first.shape[0]
        heads = w_query.shape[2]
        tail = REACH // CHUNK
        halos = 2 * LAYERS * tail + 1
        copies = LAYERS * (rows // PAIR) * 8
        anywhere = pl.BlockSpec(memory_space=pl.ANY)
        vmem = pl.BlockSpec(memory_space=pltpu.VMEM)
        return pl.pallas_call(
            functools.partial(kernel, sp_n, tp_n),
            out_shape=jax.ShapeDtypeStruct((rows, cols), BF),
            in_specs=[anywhere, vmem, vmem, anywhere, anywhere, anywhere, vmem, anywhere, anywhere],
            out_specs=anywhere,
            scratch_shapes=[
                pltpu.VMEM((rows, width), BF),
                pltpu.VMEM((CHUNK, width), BF),
                pltpu.VMEM((LAYERS, width, 3 * heads), BF),
                pltpu.VMEM((depth, width), BF),
                pltpu.VMEM((depth, cols), BF),
                pltpu.VMEM((2, rows, heads), BF),
                pltpu.VMEM((rows, 128), BF),
                pltpu.VMEM((LAYERS, REACH + rows, heads), BF),
                pltpu.VMEM((REACH + rows, 128), BF),
                pltpu.VMEM((LAYERS, (REACH + rows) // 128, heads, 128), BF),
                pltpu.VMEM((LAYERS, tp_n, rows, heads), BF),
                pltpu.VMEM((LAYERS, 256, 2 * PAIR), F32),
                pltpu.VMEM((rows // 128, 128), jnp.int32),
                pltpu.VMEM((rows, cols), BF),
                pltpu.SemaphoreType.DMA((3 * LAYERS + rows // CHUNK + 2,)),
                pltpu.SemaphoreType.DMA((rows // CHUNK,)),
                pltpu.SemaphoreType.DMA((halos,)),
                pltpu.SemaphoreType.DMA((halos,)),
                pltpu.SemaphoreType.DMA((copies,)),
                pltpu.SemaphoreType.DMA((copies,)),
            ],
            compiler_params=pltpu.CompilerParams(
                collective_id=0, has_side_effects=True, vmem_limit_bytes=60 * 1024 * 1024
            ),
        )(
            tokens,
            doc_ids.reshape(rows // 128, 128),
            gains,
            w_query,
            w_key,
            w_value,
            rel_table,
            out_first,
            out_last,
        )

    placed = (
        P(("grp", "sp"), None),
        P(("grp", "sp")),
        P(),
        P(None, None, "tp"),
        P(None, None, "tp"),
        P(None, None, "tp"),
        P(None, "tp", None),
        P(),
        P(None, "tp"),
    )
    return jax.shard_map(
        shards, mesh=mesh, in_specs=placed, out_specs=P(("grp", "sp"), "tp"), check_vma=False
    )
```

```python
import functools
import math

import jax
import jax.numpy as jnp
from jax import lax
from jax.experimental import pallas as pl
from jax.experimental.pallas import tpu as pltpu
from jax.sharding import PartitionSpec as P

SEG = 64
PREV_SEGS = 8
MAX_REL = 128
LAYERS = 2
HEAD_DIM = 64
REACH = SEG * PREV_SEGS
PAIR = 2 * SEG
WIN = REACH + PAIR
CHUNK = 2 * PAIR
BIG = 1e30
DIRECT = (7, 6, 1, 0)
LOG2E = math.log2(math.e)
MESH = pl.DeviceIdType.MESH
BF = jnp.bfloat16
F32 = jnp.float32


def scoped(f):
    @functools.wraps(f)
    def inner(*which, **named):
        with jax.named_scope("_".join([f.__name__, *map(str, which[:4])])):
            return f(*which, **named)

    return inner


def kernel(
    sp_n,
    tp_n,
    tokens,
    docs_in,
    gains_in,
    w_query,
    w_key,
    w_value,
    table_in,
    out_first,
    out_last,
    mixed,
    docs,
    gains,
    table,
    h,
    lhs,
    wqkv,
    wfirst,
    wlast,
    qbuf,
    qext,
    kbuf,
    kext,
    vt,
    att,
    bias,
    halo_docs,
    load_sem,
    halo_send,
    halo_recv,
    ag_send,
    near_recv,
    far_recv,
    partner_recv,
):
    rows, width = h.shape
    cols = wlast.shape[1]
    pairs = rows // PAIR
    chunks = rows // CHUNK
    tail = REACH // CHUNK
    sp = lax.axis_index("sp")
    me = lax.axis_index("tp")
    succ = {"sp": lax.rem(sp + 1, sp_n)}
    pred = {"sp": lax.rem(sp + sp_n - 1, sp_n)}
    left_i = lax.rem(me + tp_n - 2, tp_n)
    right_i = lax.rem(me + 2, tp_n)
    far_i = lax.rem(me + 4, tp_n)
    partner_i = me + 1 - 2 * lax.rem(me, 2)
    left, right, far, partner = {"tp": left_i}, {"tp": right_i}, {"tp": far_i}, {"tp": partner_i}
    order = list(range(chunks))[::-1]

    loads = {}

    def load(name, *pairs_of_refs, whole=None):
        sem = load_sem.at[len(loads)]
        for src, dst in pairs_of_refs:
            copy = pltpu.make_async_copy(src, dst, sem)
            copy.start()
        if whole is not None:
            copy = pltpu.make_async_copy(whole, whole, sem)
        loads[name] = copy

    def load_w(layer):
        load(
            ("w", layer),
            *(
                (w.at[layer], wqkv.at[layer, :, pl.ds(i * 128, 128)])
                for i, w in enumerate((w_query, w_key, w_value))
            ),
            whole=wqkv.at[layer],
        )

    def chunk_rows(c):
        return pl.ds(c * CHUNK, CHUNK)

    def load_tokens(c):
        load(("t", c), (tokens.at[chunk_rows(c)], h.at[chunk_rows(c)]))

    load("docs", (docs_in, docs))
    load("gains", (gains_in, gains))
    load("table", (table_in, table))
    load_tokens(order[0])
    load_w(0)
    for c in order[1:]:
        load_tokens(c)
    load("first", (out_first, wfirst))
    load_w(1)
    load("last", (out_last, wlast))

    barrier = pltpu.get_barrier_semaphore()
    for other in (left, right, far, partner):
        pl.semaphore_signal(barrier, inc=1, device_id=other, device_id_type=MESH)

    @pl.when(sp < sp_n - 1)
    def _():
        pl.semaphore_signal(barrier, inc=1, device_id=succ, device_id_type=MESH)

    @pl.when(sp > 0)
    def _():
        pl.semaphore_signal(barrier, inc=1, device_id=pred, device_id_type=MESH)

    lane = lax.broadcasted_iota(jnp.int32, (PAIR, 128), 1)
    lane_f = lane.astype(F32)

    def doc_columns(row):
        return jnp.broadcast_to(row.astype(F32), (128, 128)).T

    def build_docs():
        for b in range(rows // 128):
            col = doc_columns(docs[b : b + 1, :])
            same = col == lane_f
            kext[pl.ds(REACH + 128 * b, 128), :] = jnp.where(same, 1.0, 0.0).astype(BF)
            qext[pl.ds(128 * b, 128), :] = jnp.where(same, 0.0, -BIG).astype(BF)

    def build_halo_docs():
        void = jnp.where(sp == 0, 1.0, 0.0).astype(F32)
        for b in range(REACH // 128):
            r = (rows - REACH) // 128 + b
            col = doc_columns(halo_docs[r : r + 1, :])
            one_hot = jnp.where(col == lane_f, 1.0, 0.0)
            kext[pl.ds(128 * b, 128), :] = jnp.where(lane == 127, void, one_hot).astype(BF)

    def build_bias(layer):
        row = lax.broadcasted_iota(jnp.int32, (PAIR, PAIR), 0)
        col = lax.broadcasted_iota(jnp.int32, (PAIR, PAIR), 1)
        for n in range(2):
            near = table[layer, n : n + 1, 0 : 2 * MAX_REL]
            edge = table[layer, n : n + 1, 2 * MAX_REL : 2 * MAX_REL + 1]
            near = (near - edge) * LOG2E
            upper = jnp.concatenate([near[:, 128:], jnp.zeros((1, 128), F32)], axis=1)
            for part, values in ((0, upper), (1, near)):
                turned = pltpu.roll(
                    jnp.broadcast_to(values, (128, 256)), 128, 1, stride=1, stride_axis=0
                )[:, :128]
                if part == 1:
                    turned = jnp.where((row >= SEG) & (col < SEG), -BIG, turned)
                bias[layer, pl.ds(128 * part, 128), pl.ds(128 * n, 128)] = turned

    def project_qkv(layer, c, square_sum):
        scale = lax.rsqrt(square_sum * (1.0 / width) + 1e-06)
        qkv = jnp.dot(lhs[...], wqkv[layer], preferred_element_type=F32)
        q = qkv[:, 0:128] * (scale * (HEAD_DIM**-0.5 * LOG2E))
        k = qkv[:, 128:256] * scale
        v = qkv[:, 256:384] * scale
        wide = lax.broadcasted_iota(jnp.int32, (CHUNK, 128), 1)
        qbuf[0, chunk_rows(c), :] = jnp.where(wide < HEAD_DIM, q, 0.0).astype(BF)
        qbuf[1, chunk_rows(c), :] = jnp.where(wide < HEAD_DIM, 0.0, q).astype(BF)
        kbuf[layer, pl.ds(REACH + CHUNK * c, CHUNK), :] = k.astype(BF)
        for i in range(2):
            block = v[128 * i : 128 * (i + 1), :].T
            vt[layer, REACH // 128 + 2 * c + i] = block.astype(BF)

    def gain_row(layer, n, step):
        return gains[layer : layer + 1, pl.ds(n * step, step)].astype(F32)

    @scoped
    def dense(c):
        step = 256
        total = jnp.zeros((CHUNK, 128), F32)
        for n in range(width // step):
            x = h[chunk_rows(c), pl.ds(n * step, step)].astype(F32)
            square = x * x
            for j in range(step // 128):
                total = total + square[:, 128 * j : 128 * (j + 1)]
            lhs[:, pl.ds(n * step, step)] = (x * gain_row(0, n, step)).astype(BF)
        project_qkv(0, c, jnp.sum(total, axis=1, keepdims=True))

    def attended_rows(layer, c):
        return jnp.concatenate([att[layer, t, chunk_rows(c), :] for t in range(tp_n)], axis=1)

    @scoped
    def trans(c, between=None):
        step = 256
        a = attended_rows(0, c)
        total = jnp.zeros((CHUNK, 128), F32)
        for n in range(width // step):
            part = pl.ds(n * step, step)
            update = jnp.dot(a, wfirst[:, part], preferred_element_type=F32)
            x = (h[chunk_rows(c), part].astype(F32) + update).astype(BF)
            h[chunk_rows(c), part] = x
            x = x.astype(F32)
            square = x * x
            for j in range(step // 128):
                total = total + square[:, 128 * j : 128 * (j + 1)]
            lhs[:, part] = (x * gain_row(1, n, step)).astype(BF)
            if between is not None and n == width // step // 2 - 1:
                between()
        project_qkv(1, c, jnp.sum(total, axis=1, keepdims=True))

    @scoped
    def final(c):
        a = attended_rows(1, c)
        update = jnp.dot(a, wlast[...], preferred_element_type=F32)
        own = h[chunk_rows(c), pl.ds(pl.multiple_of(me * cols, cols), cols)].astype(F32)
        mixed[chunk_rows(c), :] = (own + update).astype(BF)

    def scores_of(layer, p):
        window = pl.ds(PAIR * p, WIN)
        mine = pl.ds(PAIR * p, PAIR)
        keys = jnp.concatenate([kbuf[layer, window, :], kext[window, :]], axis=1)
        queries = jnp.concatenate(
            [
                jnp.concatenate([qbuf[0, mine, :], qext[mine, :]], axis=1),
                jnp.concatenate([qbuf[1, mine, :], qext[mine, :]], axis=1),
            ],
            axis=0,
        )
        s = lax.dot_general(
            keys, queries, (((1,), (1,)), ((), ())), preferred_element_type=F32
        )
        first = lax.broadcasted_iota(jnp.int32, (SEG, 2 * PAIR), 1)
        s_first = jnp.where(lax.rem(first, PAIR) < SEG, s[:SEG], -BIG)
        return jnp.concatenate(
            [s_first, s[SEG : WIN - 256], s[WIN - 256 :] + bias[layer]], axis=0
        )

    def weigh(layer, p, s):
        e = jnp.exp2(s - jnp.max(s, axis=0, keepdims=True))
        inverse = 1.0 / jnp.sum(e, axis=0, keepdims=True)
        values = jnp.concatenate([vt[layer, p + i] for i in range(WIN // 128)], axis=1)
        o = jnp.dot(values, e.astype(BF), preferred_element_type=F32)
        o = jnp.concatenate(
            [
                o[:HEAD_DIM, :PAIR] * inverse[:, :PAIR],
                o[HEAD_DIM:, PAIR:] * inverse[:, PAIR:],
            ],
            axis=0,
        )
        att[layer, me, pl.ds(PAIR * p, PAIR), :] = o.T.astype(BF)

    @scoped
    def attend(layer, *which):
        scores = [scores_of(layer, p) for p in which]
        for p, s in zip(which, scores):
            weigh(layer, p, s)

    def remote(src, dst, send_sem, recv_sem, device):
        return pltpu.make_async_remote_copy(
            src_ref=src,
            dst_ref=dst,
            send_sem=send_sem,
            recv_sem=recv_sem,
            device_id=device,
            device_id_type=MESH,
        )

    def halo(layer, c):
        i = layer * tail + c - (chunks - tail)
        k0 = CHUNK * (c - (chunks - tail))
        b0 = k0 // 128
        return (
            remote(
                kbuf.at[layer, pl.ds(REACH + CHUNK * c, CHUNK)],
                kbuf.at[layer, pl.ds(k0, CHUNK)],
                halo_send.at[2 * i],
                halo_recv.at[2 * i],
                succ,
            ),
            remote(
                vt.at[layer, pl.ds(REACH // 128 + 2 * c, 2)],
                vt.at[layer, pl.ds(b0, 2)],
                halo_send.at[2 * i + 1],
                halo_recv.at[2 * i + 1],
                succ,
            ),
        )

    def doc_halo():
        i = 2 * LAYERS * tail
        return remote(docs, halo_docs, halo_send.at[i], halo_recv.at[i], succ)

    halos = []

    def send_halo(layer, c):
        halos.extend(halo(layer, c))

        @pl.when(sp < sp_n - 1)
        def _():
            for copy in halo(layer, c):
                copy.start()

    @scoped
    def wait_halo(layer, c):
        @pl.when(sp > 0)
        def _():
            for copy in halo(layer, c):
                copy.wait_recv()

    sent = [0] * LAYERS

    def send(layer, p, slot, device, recv_sem, part=None):
        first = PAIR * p + (SEG if part == 1 else 0)
        count = PAIR if part is None else SEG
        ref = att.at[layer, slot, pl.ds(first, count)]
        remote(ref, ref, ag_send.at[layer], recv_sem, device).start()
        sent[layer] += count

    def arrived(layer, slots, count, recv_sem):
        ref = att.at[layer, 0:slots, pl.ds(0, count)]
        remote(ref, ref, ag_send.at[layer], recv_sem, partner).wait_recv()

    def near_sem(layer, p):
        return near_recv.at[layer * pairs + p]

    def far_sem(layer, p):
        return far_recv.at[layer * pairs + p]

    def partner_sem(layer, p):
        return partner_recv.at[layer * chunks + p // 2]

    def is_direct(layer, p):
        return layer == 0 or p in DIRECT

    def send_own(layer, p):
        send(layer, p, me, right, near_sem(layer, p))
        send(layer, p, me, left, near_sem(layer, p))
        if is_direct(layer, p):
            send(layer, p, me, far, far_sem(layer, p))
        send(layer, p, me, partner, partner_sem(layer, p))

    @scoped
    def near(layer, *which):
        for p in which:
            arrived(layer, 2, PAIR, near_sem(layer, p))
            if not is_direct(layer, p):
                send(layer, p, left_i, right, far_sem(layer, p), 0)
                send(layer, p, right_i, left, far_sem(layer, p), 1)
            send(layer, p, left_i, partner, partner_sem(layer, p))
            send(layer, p, right_i, partner, partner_sem(layer, p))

    @scoped
    def distant(layer, *which):
        for p in which:
            arrived(layer, 1, PAIR, far_sem(layer, p))
            send(layer, p, far_i, partner, partner_sem(layer, p))

    @scoped
    def consume(layer, c):
        arrived(layer, tp_n, PAIR, partner_sem(layer, 2 * c))

    def attend_send(layer, *which):
        attend(layer, *which)
        for p in which:
            send_own(layer, p)

    @pl.when(sp == 0)
    def _():
        for layer in range(LAYERS):
            kbuf[layer, 0:REACH, :] = jnp.zeros((REACH, 128), BF)
            for b in range(REACH // 128):
                vt[layer, b] = jnp.zeros((128, 128), BF)
        halo_docs[...] = jnp.zeros(halo_docs.shape, jnp.int32)

    loads["docs"].wait()
    build_docs()
    loads["table"].wait()
    build_bias(0)
    loads["gains"].wait()
    loads[("w", 0)].wait()
    c3, c2, c1, c0 = order
    loads[("t", c3)].wait()
    dense(c3)
    with jax.named_scope("barrier"):
        pl.semaphore_wait(barrier, 4 + jnp.where(sp > 0, 1, 0) + jnp.where(sp < sp_n - 1, 1, 0))
    send_halo(0, c3)

    @pl.when(sp < sp_n - 1)
    def _():
        doc_halo().start()

    loads[("t", c2)].wait()
    dense(c2)
    send_halo(0, c2)
    loads[("t", c1)].wait()
    dense(c1)
    attend_send(0, 7, 6)
    loads[("t", c0)].wait()
    dense(c0)
    attend_send(0, 5, 4)

    @pl.when(sp > 0)
    def _():
        doc_halo().wait_recv()

    build_halo_docs()
    wait_halo(0, c3)
    attend_send(0, 3, 2)
    build_bias(1)
    loads["first"].wait()
    loads[("w", 1)].wait()
    loads["last"].wait()
    near(0, 7, 6)
    wait_halo(0, c2)
    attend_send(0, 1, 0)
    distant(0, 7, 6)
    near(0, 5, 4)
    consume(0, c3)

    def serve_0():
        distant(0, 5, 4)
        near(0, 3)

    def serve_1():
        near(0, 2)
        distant(0, 3, 2)

    def serve_2():
        near(0, 1, 0)
        distant(0, 1, 0)

    trans(c3, between=serve_0)
    send_halo(1, c3)
    consume(0, c2)
    trans(c2, between=serve_1)
    send_halo(1, c2)
    consume(0, c1)
    trans(c1, between=serve_2)
    attend_send(1, 7, 6)
    consume(0, c0)
    trans(c0)
    attend_send(1, 5, 4)
    near(1, 7, 6)
    wait_halo(1, c3)
    attend_send(1, 3, 2)
    distant(1, 7, 6)
    wait_halo(1, c2)
    attend_send(1, 1, 0)
    near(1, 5, 4)
    consume(1, c3)
    final(c3)
    near(1, 3, 2)
    distant(1, 5, 4)
    near(1, 1, 0)
    distant(1, 3, 2)
    consume(1, c2)
    final(c2)
    consume(1, c1)
    final(c1)
    distant(1, 1, 0)
    consume(1, c0)
    final(c0)
    with jax.named_scope("sends"):
        for layer in range(LAYERS):
            whole, rest = divmod(sent[layer], rows)
            ref = att.at[layer, 0:whole]
            remote(ref, ref, ag_send.at[layer], near_sem(layer, 0), partner).wait_send()
            if rest:
                ref = att.at[layer, 0, pl.ds(0, rest)]
                remote(ref, ref, ag_send.at[layer], near_sem(layer, 0), partner).wait_send()

        @pl.when(sp < sp_n - 1)
        def _():
            doc_halo().wait_send()
            for copy in halos:
                copy.wait_send()


def solution(mesh):
    sp_n, tp_n = mesh.shape["sp"], mesh.shape["tp"]

    def shards(tokens, doc_ids, gains, w_query, w_key, w_value, rel_table, out_first, out_last):
        rows, width = tokens.shape
        cols = out_last.shape[1]
        depth = out_first.shape[0]
        heads = w_query.shape[2]
        tail = REACH // CHUNK
        halos = 2 * LAYERS * tail + 1
        anywhere = pl.BlockSpec(memory_space=pltpu.HBM)
        vmem = pl.BlockSpec(memory_space=pltpu.VMEM)
        return pl.pallas_call(
            functools.partial(kernel, sp_n, tp_n),
            out_shape=jax.ShapeDtypeStruct((rows, cols), BF),
            in_specs=[anywhere] * 9,
            out_specs=vmem,
            scratch_shapes=[
                pltpu.VMEM((rows // 128, 128), jnp.int32),
                pltpu.VMEM(gains.shape, gains.dtype),
                pltpu.VMEM(rel_table.shape, rel_table.dtype),
                pltpu.VMEM((rows, width), BF),
                pltpu.VMEM((CHUNK, width), BF),
                pltpu.VMEM((LAYERS, width, 3 * heads), BF),
                pltpu.VMEM((depth, width), BF),
                pltpu.VMEM((depth, cols), BF),
                pltpu.VMEM((2, rows, heads), BF),
                pltpu.VMEM((rows, 128), BF),
                pltpu.VMEM((LAYERS, REACH + rows, heads), BF),
                pltpu.VMEM((REACH + rows, 128), BF),
                pltpu.VMEM((LAYERS, (REACH + rows) // 128, heads, 128), BF),
                pltpu.VMEM((LAYERS, tp_n, rows, heads), BF),
                pltpu.VMEM((LAYERS, 256, 2 * PAIR), F32),
                pltpu.VMEM((rows // 128, 128), jnp.int32),
                pltpu.SemaphoreType.DMA((LAYERS + rows // CHUNK + 5,)),
                pltpu.SemaphoreType.DMA((halos,)),
                pltpu.SemaphoreType.DMA((halos,)),
                pltpu.SemaphoreType.DMA((LAYERS,)),
                pltpu.SemaphoreType.DMA((LAYERS * (rows // PAIR),)),
                pltpu.SemaphoreType.DMA((LAYERS * (rows // PAIR),)),
                pltpu.SemaphoreType.DMA((LAYERS * (rows // CHUNK),)),
            ],
            compiler_params=pltpu.CompilerParams(
                collective_id=0, has_side_effects=True, vmem_limit_bytes=60 * 1024 * 1024
            ),
        )(
            tokens,
            doc_ids.reshape(rows // 128, 128),
            gains,
            w_query,
            w_key,
            w_value,
            rel_table,
            out_first,
            out_last,
        )

    placed = (
        P(("grp", "sp"), None),
        P(("grp", "sp")),
        P(),
        P(None, None, "tp"),
        P(None, None, "tp"),
        P(None, None, "tp"),
        P(None, "tp", None),
        P(),
        P(None, "tp"),
    )
    return jax.shard_map(
        shards, mesh=mesh, in_specs=placed, out_specs=P(("grp", "sp"), "tp"), check_vma=False
    )
```

```python
import functools
import math

import jax
import jax.numpy as jnp
from jax import lax
from jax.experimental import pallas as pl
from jax.experimental.pallas import tpu as pltpu
from jax.sharding import PartitionSpec as P

SEG = 64
PREV_SEGS = 8
MAX_REL = 128
LAYERS = 2
HEAD_DIM = 64
REACH = SEG * PREV_SEGS
PAIR = 2 * SEG
WIN = REACH + PAIR
CHUNK = 2 * PAIR
BIG = 1e30
DIRECT = (7, 6, 1, 0)
LOG2E = math.log2(math.e)
MESH = pl.DeviceIdType.MESH
BF = jnp.bfloat16
F32 = jnp.float32


def scoped(f):
    @functools.wraps(f)
    def inner(*which, **named):
        with jax.named_scope("_".join([f.__name__, *map(str, which[:4])])):
            return f(*which, **named)

    return inner


def kernel(
    sp_n,
    tp_n,
    tokens,
    docs_in,
    gains_in,
    w_query,
    w_key,
    w_value,
    table_in,
    out_first,
    out_last,
    mixed,
    docs,
    gains,
    table,
    h,
    lhs,
    wqkv,
    wfirst,
    wlast,
    qbuf,
    qext,
    kbuf,
    kext,
    vt,
    att,
    bias,
    halo_docs,
    load_sem,
    halo_send,
    halo_recv,
    ag_send,
    near_recv,
    far_recv,
    partner_recv,
):
    rows, width = h.shape
    cols = wlast.shape[1]
    pairs = rows // PAIR
    chunks = rows // CHUNK
    tail = REACH // CHUNK
    sp = lax.axis_index("sp")
    me = lax.axis_index("tp")
    succ = {"sp": lax.rem(sp + 1, sp_n)}
    pred = {"sp": lax.rem(sp + sp_n - 1, sp_n)}
    left_i = lax.rem(me + tp_n - 2, tp_n)
    right_i = lax.rem(me + 2, tp_n)
    far_i = lax.rem(me + 4, tp_n)
    partner_i = me + 1 - 2 * lax.rem(me, 2)
    left, right, far, partner = {"tp": left_i}, {"tp": right_i}, {"tp": far_i}, {"tp": partner_i}
    order = list(range(chunks))[::-1]

    loads = {}

    def load(name, *pairs_of_refs, whole=None):
        sem = load_sem.at[len(loads)]
        for src, dst in pairs_of_refs:
            copy = pltpu.make_async_copy(src, dst, sem)
            copy.start()
        if whole is not None:
            copy = pltpu.make_async_copy(whole, whole, sem)
        loads[name] = copy

    def load_w(layer):
        load(
            ("w", layer),
            *(
                (w.at[layer], wqkv.at[layer, :, pl.ds(i * 128, 128)])
                for i, w in enumerate((w_query, w_key, w_value))
            ),
            whole=wqkv.at[layer],
        )

    def chunk_rows(c):
        return pl.ds(c * CHUNK, CHUNK)

    def load_tokens(c):
        load(("t", c), (tokens.at[chunk_rows(c)], h.at[chunk_rows(c)]))

    load("docs", (docs_in, docs))
    load("gains", (gains_in, gains))
    load("table", (table_in, table))
    load_tokens(order[0])
    load_w(0)
    for c in order[1:]:
        load_tokens(c)
    barrier = pltpu.get_barrier_semaphore()
    for other in (left, right, far, partner):
        pl.semaphore_signal(barrier, inc=1, device_id=other, device_id_type=MESH)

    @pl.when(sp < sp_n - 1)
    def _():
        pl.semaphore_signal(barrier, inc=1, device_id=succ, device_id_type=MESH)

    @pl.when(sp > 0)
    def _():
        pl.semaphore_signal(barrier, inc=1, device_id=pred, device_id_type=MESH)

    lane = lax.broadcasted_iota(jnp.int32, (PAIR, 128), 1)
    lane_f = lane.astype(F32)

    def doc_columns(row):
        return jnp.broadcast_to(row.astype(F32), (128, 128)).T

    def build_docs():
        for b in range(rows // 128):
            col = doc_columns(docs[b : b + 1, :])
            same = col == lane_f
            kext[pl.ds(REACH + 128 * b, 128), :] = jnp.where(same, 1.0, 0.0).astype(BF)
            qext[pl.ds(128 * b, 128), :] = jnp.where(same, 0.0, -BIG).astype(BF)

    def build_halo_docs():
        void = jnp.where(sp == 0, 1.0, 0.0).astype(F32)
        for b in range(REACH // 128):
            r = (rows - REACH) // 128 + b
            col = doc_columns(halo_docs[r : r + 1, :])
            one_hot = jnp.where(col == lane_f, 1.0, 0.0)
            kext[pl.ds(128 * b, 128), :] = jnp.where(lane == 127, void, one_hot).astype(BF)

    def build_bias(layer):
        row = lax.broadcasted_iota(jnp.int32, (PAIR, PAIR), 0)
        col = lax.broadcasted_iota(jnp.int32, (PAIR, PAIR), 1)
        for n in range(2):
            near = table[layer, n : n + 1, 0 : 2 * MAX_REL]
            edge = table[layer, n : n + 1, 2 * MAX_REL : 2 * MAX_REL + 1]
            near = (near - edge) * LOG2E
            upper = jnp.concatenate([near[:, 128:], jnp.zeros((1, 128), F32)], axis=1)
            for part, values in ((0, upper), (1, near)):
                turned = pltpu.roll(
                    jnp.broadcast_to(values, (128, 256)), 128, 1, stride=1, stride_axis=0
                )[:, :128]
                if part == 1:
                    turned = jnp.where((row >= SEG) & (col < SEG), -BIG, turned)
                bias[layer, pl.ds(128 * part, 128), pl.ds(128 * n, 128)] = turned

    def project_qkv(layer, c, square_sum):
        scale = lax.rsqrt(square_sum * (1.0 / width) + 1e-06)
        qkv = jnp.dot(lhs[...], wqkv[layer], preferred_element_type=F32)
        q = qkv[:, 0:128] * (scale * (HEAD_DIM**-0.5 * LOG2E))
        k = qkv[:, 128:256] * scale
        v = qkv[:, 256:384] * scale
        wide = lax.broadcasted_iota(jnp.int32, (CHUNK, 128), 1)
        qbuf[0, chunk_rows(c), :] = jnp.where(wide < HEAD_DIM, q, 0.0).astype(BF)
        qbuf[1, chunk_rows(c), :] = jnp.where(wide < HEAD_DIM, 0.0, q).astype(BF)
        kbuf[layer, pl.ds(REACH + CHUNK * c, CHUNK), :] = k.astype(BF)
        for i in range(2):
            block = v[128 * i : 128 * (i + 1), :].T
            vt[layer, REACH // 128 + 2 * c + i] = block.astype(BF)

    def gain_row(layer, n, step):
        return gains[layer : layer + 1, pl.ds(n * step, step)].astype(F32)

    @scoped
    def dense(c):
        step = 256
        total = jnp.zeros((CHUNK, 128), F32)
        for n in range(width // step):
            x = h[chunk_rows(c), pl.ds(n * step, step)].astype(F32)
            square = x * x
            for j in range(step // 128):
                total = total + square[:, 128 * j : 128 * (j + 1)]
            lhs[:, pl.ds(n * step, step)] = (x * gain_row(0, n, step)).astype(BF)
        project_qkv(0, c, jnp.sum(total, axis=1, keepdims=True))

    @scoped
    def trans(c, between=None):
        step = 256
        a = jnp.concatenate([att[0, t, chunk_rows(c), :] for t in range(tp_n)], axis=1)
        total = jnp.zeros((CHUNK, 128), F32)
        for n in range(width // step):
            part = pl.ds(n * step, step)
            update = jnp.dot(a, wfirst[:, part], preferred_element_type=F32)
            x = (h[chunk_rows(c), part].astype(F32) + update).astype(BF)
            h[chunk_rows(c), part] = x
            x = x.astype(F32)
            square = x * x
            for j in range(step // 128):
                total = total + square[:, 128 * j : 128 * (j + 1)]
            lhs[:, part] = (x * gain_row(1, n, step)).astype(BF)
            if between is not None and n == width // step // 2 - 1:
                between()
        project_qkv(1, c, jnp.sum(total, axis=1, keepdims=True))

    @scoped
    def final(c, count=1):
        mine = pl.ds(c * CHUNK, count * CHUNK)
        a = jnp.concatenate([att[1, t, mine, :] for t in range(tp_n)], axis=1)
        update = jnp.dot(a, wlast[...], preferred_element_type=F32)
        own = h[mine, pl.ds(pl.multiple_of(me * cols, cols), cols)].astype(F32)
        mixed[mine, :] = (own + update).astype(BF)

    def scores_of(layer, p):
        window = pl.ds(PAIR * p, WIN)
        mine = pl.ds(PAIR * p, PAIR)
        keys = jnp.concatenate([kbuf[layer, window, :], kext[window, :]], axis=1)
        queries = jnp.concatenate(
            [
                jnp.concatenate([qbuf[0, mine, :], qext[mine, :]], axis=1),
                jnp.concatenate([qbuf[1, mine, :], qext[mine, :]], axis=1),
            ],
            axis=0,
        )
        s = lax.dot_general(
            keys, queries, (((1,), (1,)), ((), ())), preferred_element_type=F32
        )
        first = lax.broadcasted_iota(jnp.int32, (SEG, 2 * PAIR), 1)
        s_first = jnp.where(lax.rem(first, PAIR) < SEG, s[:SEG], -BIG)
        return jnp.concatenate(
            [s_first, s[SEG : WIN - 256], s[WIN - 256 :] + bias[layer]], axis=0
        )

    def weigh(layer, p, s):
        e = jnp.exp2(s - jnp.max(s, axis=0, keepdims=True))
        inverse = 1.0 / jnp.sum(e, axis=0, keepdims=True)
        values = jnp.concatenate([vt[layer, p + i] for i in range(WIN // 128)], axis=1)
        o = jnp.dot(values, e.astype(BF), preferred_element_type=F32)
        o = jnp.concatenate(
            [
                o[:HEAD_DIM, :PAIR] * inverse[:, :PAIR],
                o[HEAD_DIM:, PAIR:] * inverse[:, PAIR:],
            ],
            axis=0,
        )
        att[layer, me, pl.ds(PAIR * p, PAIR), :] = o.T.astype(BF)

    @scoped
    def attend(layer, *which):
        scores = [scores_of(layer, p) for p in which]
        for p, s in zip(which, scores):
            weigh(layer, p, s)

    def remote(src, dst, send_sem, recv_sem, device):
        return pltpu.make_async_remote_copy(
            src_ref=src,
            dst_ref=dst,
            send_sem=send_sem,
            recv_sem=recv_sem,
            device_id=device,
            device_id_type=MESH,
        )

    def halo(layer, c):
        i = layer * tail + c - (chunks - tail)
        k0 = CHUNK * (c - (chunks - tail))
        b0 = k0 // 128
        return (
            remote(
                kbuf.at[layer, pl.ds(REACH + CHUNK * c, CHUNK)],
                kbuf.at[layer, pl.ds(k0, CHUNK)],
                halo_send.at[2 * i],
                halo_recv.at[2 * i],
                succ,
            ),
            remote(
                vt.at[layer, pl.ds(REACH // 128 + 2 * c, 2)],
                vt.at[layer, pl.ds(b0, 2)],
                halo_send.at[2 * i + 1],
                halo_recv.at[2 * i + 1],
                succ,
            ),
        )

    def doc_halo():
        i = 2 * LAYERS * tail
        return remote(docs, halo_docs, halo_send.at[i], halo_recv.at[i], succ)

    halos = []

    def send_halo(layer, c):
        halos.extend(halo(layer, c))

        @pl.when(sp < sp_n - 1)
        def _():
            for copy in halo(layer, c):
                copy.start()

    @scoped
    def wait_halo(layer, c):
        @pl.when(sp > 0)
        def _():
            for copy in halo(layer, c):
                copy.wait_recv()

    sent = [0] * LAYERS

    def send(layer, p, slot, device, recv_sem, part=None):
        first = PAIR * p + (SEG if part == 1 else 0)
        count = PAIR if part is None else SEG
        ref = att.at[layer, slot, pl.ds(first, count)]
        remote(ref, ref, ag_send.at[layer], recv_sem, device).start()
        sent[layer] += count

    def arrived(layer, slots, count, recv_sem):
        ref = att.at[layer, 0:slots, pl.ds(0, count)]
        remote(ref, ref, ag_send.at[layer], recv_sem, partner).wait_recv()

    def near_sem(layer, p):
        return near_recv.at[layer * pairs + p]

    def far_sem(layer, p):
        return far_recv.at[layer * pairs + p]

    def partner_sem(layer, p):
        return partner_recv.at[layer * chunks + p // 2]

    def is_direct(layer, p):
        return layer == 0 or p in DIRECT

    def send_own(layer, p):
        if is_direct(layer, p):
            send(layer, p, me, far, far_sem(layer, p))
        send(layer, p, me, right, near_sem(layer, p))
        send(layer, p, me, left, near_sem(layer, p))
        send(layer, p, me, partner, partner_sem(layer, p))

    @scoped
    def near(layer, *which):
        for p in which:
            arrived(layer, 2, PAIR, near_sem(layer, p))
            if not is_direct(layer, p):
                send(layer, p, left_i, right, far_sem(layer, p), 0)
                send(layer, p, right_i, left, far_sem(layer, p), 1)
            send(layer, p, left_i, partner, partner_sem(layer, p))
            send(layer, p, right_i, partner, partner_sem(layer, p))

    @scoped
    def distant(layer, *which):
        for p in which:
            arrived(layer, 1, PAIR, far_sem(layer, p))
            send(layer, p, far_i, partner, partner_sem(layer, p))

    @scoped
    def consume(layer, c):
        arrived(layer, tp_n, PAIR, partner_sem(layer, 2 * c))

    def attend_send(layer, *which):
        attend(layer, *which)
        for p in which:
            send_own(layer, p)

    @pl.when(sp == 0)
    def _():
        for layer in range(LAYERS):
            kbuf[layer, 0:REACH, :] = jnp.zeros((REACH, 128), BF)
            for b in range(REACH // 128):
                vt[layer, b] = jnp.zeros((128, 128), BF)
        halo_docs[...] = jnp.zeros(halo_docs.shape, jnp.int32)

    loads["docs"].wait()
    build_docs()
    loads["table"].wait()
    build_bias(0)
    loads["gains"].wait()
    loads[("w", 0)].wait()
    c3, c2, c1, c0 = order
    loads[("t", c3)].wait()
    dense(c3)
    load("first", (out_first, wfirst))
    load_w(1)
    load("last", (out_last, wlast))
    loads[("t", c2)].wait()
    dense(c2)
    with jax.named_scope("barrier"):
        pl.semaphore_wait(barrier, 4 + jnp.where(sp > 0, 1, 0) + jnp.where(sp < sp_n - 1, 1, 0))
    send_halo(0, c3)

    @pl.when(sp < sp_n - 1)
    def _():
        doc_halo().start()

    send_halo(0, c2)
    loads[("t", c1)].wait()
    dense(c1)
    attend_send(0, 7, 6)
    loads[("t", c0)].wait()
    dense(c0)
    attend_send(0, 5, 4)

    @pl.when(sp > 0)
    def _():
        doc_halo().wait_recv()

    build_halo_docs()
    wait_halo(0, c3)
    attend(0, 3, 2)
    near(0, 7, 6)
    distant(0, 7, 6)
    send_own(0, 3)
    send_own(0, 2)
    build_bias(1)
    loads["first"].wait()
    loads[("w", 1)].wait()
    loads["last"].wait()
    wait_halo(0, c2)
    attend_send(0, 1, 0)
    consume(0, c3)

    def serve(*which):
        near(0, *which)
        distant(0, *which)

    trans(c3, between=functools.partial(serve, 5, 4))
    send_halo(1, c3)
    consume(0, c2)
    trans(c2, between=functools.partial(serve, 3, 2))
    send_halo(1, c2)
    consume(0, c1)
    trans(c1)
    serve(1, 0)
    attend_send(1, 7, 6)
    consume(0, c0)
    trans(c0)
    attend_send(1, 5, 4)
    wait_halo(1, c3)
    attend_send(1, 3, 2)
    wait_halo(1, c2)
    attend_send(1, 1, 0)
    near(1, 7, 6)
    distant(1, 7, 6)
    near(1, 5, 4)
    near(1, 3, 2)
    consume(1, c3)
    final(c3)
    near(1, 1, 0)
    distant(1, 1, 0)
    consume(1, c0)
    final(c0)
    distant(1, 5, 4)
    distant(1, 3, 2)
    consume(1, c2)
    consume(1, c1)
    final(c1, 2)
    with jax.named_scope("sends"):
        for layer in range(LAYERS):
            whole, rest = divmod(sent[layer], rows)
            ref = att.at[layer, 0:whole]
            remote(ref, ref, ag_send.at[layer], near_sem(layer, 0), partner).wait_send()
            if rest:
                ref = att.at[layer, 0, pl.ds(0, rest)]
                remote(ref, ref, ag_send.at[layer], near_sem(layer, 0), partner).wait_send()

        @pl.when(sp < sp_n - 1)
        def _():
            doc_halo().wait_send()
            for copy in halos:
                copy.wait_send()


def solution(mesh):
    sp_n, tp_n = mesh.shape["sp"], mesh.shape["tp"]

    def shards(tokens, doc_ids, gains, w_query, w_key, w_value, rel_table, out_first, out_last):
        rows, width = tokens.shape
        cols = out_last.shape[1]
        depth = out_first.shape[0]
        heads = w_query.shape[2]
        tail = REACH // CHUNK
        halos = 2 * LAYERS * tail + 1
        anywhere = pl.BlockSpec(memory_space=pltpu.HBM)
        vmem = pl.BlockSpec(memory_space=pltpu.VMEM)
        return pl.pallas_call(
            functools.partial(kernel, sp_n, tp_n),
            out_shape=jax.ShapeDtypeStruct((rows, cols), BF),
            in_specs=[anywhere] * 9,
            out_specs=vmem,
            scratch_shapes=[
                pltpu.VMEM((rows // 128, 128), jnp.int32),
                pltpu.VMEM(gains.shape, gains.dtype),
                pltpu.VMEM(rel_table.shape, rel_table.dtype),
                pltpu.VMEM((rows, width), BF),
                pltpu.VMEM((CHUNK, width), BF),
                pltpu.VMEM((LAYERS, width, 3 * heads), BF),
                pltpu.VMEM((depth, width), BF),
                pltpu.VMEM((depth, cols), BF),
                pltpu.VMEM((2, rows, heads), BF),
                pltpu.VMEM((rows, 128), BF),
                pltpu.VMEM((LAYERS, REACH + rows, heads), BF),
                pltpu.VMEM((REACH + rows, 128), BF),
                pltpu.VMEM((LAYERS, (REACH + rows) // 128, heads, 128), BF),
                pltpu.VMEM((LAYERS, tp_n, rows, heads), BF),
                pltpu.VMEM((LAYERS, 256, 2 * PAIR), F32),
                pltpu.VMEM((rows // 128, 128), jnp.int32),
                pltpu.SemaphoreType.DMA((LAYERS + rows // CHUNK + 5,)),
                pltpu.SemaphoreType.DMA((halos,)),
                pltpu.SemaphoreType.DMA((halos,)),
                pltpu.SemaphoreType.DMA((LAYERS,)),
                pltpu.SemaphoreType.DMA((LAYERS * (rows // PAIR),)),
                pltpu.SemaphoreType.DMA((LAYERS * (rows // PAIR),)),
                pltpu.SemaphoreType.DMA((LAYERS * (rows // CHUNK),)),
            ],
            compiler_params=pltpu.CompilerParams(
                collective_id=0, has_side_effects=True, vmem_limit_bytes=40 * 1024 * 1024
            ),
        )(
            *[
                pltpu.with_memory_space_constraint(x, pltpu.HBM)
                for x in (
                    tokens,
                    doc_ids.reshape(rows // 128, 128),
                    gains,
                    w_query,
                    w_key,
                    w_value,
                    rel_table,
                    out_first,
                    out_last,
                )
            ],
        )

    placed = (
        P(("grp", "sp"), None),
        P(("grp", "sp")),
        P(),
        P(None, None, "tp"),
        P(None, None, "tp"),
        P(None, None, "tp"),
        P(None, "tp", None),
        P(),
        P(None, "tp"),
    )
    return jax.shard_map(
        shards, mesh=mesh, in_specs=placed, out_specs=P(("grp", "sp"), "tp"), check_vma=False
    )
```

```python
import functools
import math

import jax
import jax.numpy as jnp
from jax import lax
from jax.experimental import pallas as pl
from jax.experimental.pallas import tpu as pltpu
from jax.sharding import PartitionSpec as P

SEG = 64
PREV_SEGS = 8
MAX_REL = 128
LAYERS = 2
HEAD_DIM = 64
REACH = SEG * PREV_SEGS
PAIR = 2 * SEG
WIN = REACH + PAIR
CHUNK = 2 * PAIR
BIG = 1e30
DIRECT = (3, 0)
LOG2E = math.log2(math.e)
MESH = pl.DeviceIdType.MESH
BF = jnp.bfloat16
F32 = jnp.float32


def scoped(f):
    @functools.wraps(f)
    def inner(*which, **named):
        with jax.named_scope("_".join([f.__name__, *map(str, which[:4])])):
            return f(*which, **named)

    return inner


def kernel(
    sp_n,
    tp_n,
    tokens,
    docs_in,
    gains_in,
    w_query,
    w_key,
    w_value,
    table_in,
    out_first,
    out_last,
    mixed,
    docs,
    gains,
    table,
    h,
    lhs,
    wqkv,
    wfirst,
    wlast,
    qbuf,
    qext,
    kbuf,
    kext,
    vt,
    att,
    bias,
    halo_docs,
    load_sem,
    halo_send,
    halo_recv,
    ag_send,
    near_recv,
    far_recv,
    partner_recv,
):
    rows, width = h.shape
    cols = wlast.shape[1]
    chunks = rows // CHUNK
    tail = REACH // CHUNK
    sp = lax.axis_index("sp")
    me = lax.axis_index("tp")
    succ = {"sp": lax.rem(sp + 1, sp_n)}
    pred = {"sp": lax.rem(sp + sp_n - 1, sp_n)}
    left_i = lax.rem(me + tp_n - 2, tp_n)
    right_i = lax.rem(me + 2, tp_n)
    far_i = lax.rem(me + 4, tp_n)
    partner_i = me + 1 - 2 * lax.rem(me, 2)
    left, right, far, partner = {"tp": left_i}, {"tp": right_i}, {"tp": far_i}, {"tp": partner_i}
    order = list(range(chunks))[::-1]

    loads = {}

    def load(name, *pairs_of_refs, whole=None):
        sem = load_sem.at[len(loads)]
        for src, dst in pairs_of_refs:
            copy = pltpu.make_async_copy(src, dst, sem)
            copy.start()
        if whole is not None:
            copy = pltpu.make_async_copy(whole, whole, sem)
        loads[name] = copy

    def load_w(layer):
        load(
            ("w", layer),
            *(
                (w.at[layer], wqkv.at[layer, :, pl.ds(i * 128, 128)])
                for i, w in enumerate((w_query, w_key, w_value))
            ),
            whole=wqkv.at[layer],
        )

    def chunk_rows(c):
        return pl.ds(c * CHUNK, CHUNK)

    def load_tokens(c):
        load(("t", c), (tokens.at[chunk_rows(c)], h.at[chunk_rows(c)]))

    load("docs", (docs_in, docs))
    load("gains", (gains_in, gains))
    load("table", (table_in, table))
    load_tokens(order[0])
    load_w(0)
    load_tokens(order[1])
    barrier = pltpu.get_barrier_semaphore()
    for other in (left, right, far, partner):
        pl.semaphore_signal(barrier, inc=1, device_id=other, device_id_type=MESH)

    @pl.when(sp < sp_n - 1)
    def _():
        pl.semaphore_signal(barrier, inc=1, device_id=succ, device_id_type=MESH)

    @pl.when(sp > 0)
    def _():
        pl.semaphore_signal(barrier, inc=1, device_id=pred, device_id_type=MESH)

    lane = lax.broadcasted_iota(jnp.int32, (PAIR, 128), 1)
    lane_f = lane.astype(F32)

    def doc_columns(row):
        return jnp.broadcast_to(row.astype(F32), (128, 128)).T

    def build_docs():
        for b in range(rows // 128):
            col = doc_columns(docs[b : b + 1, :])
            same = col == lane_f
            kext[pl.ds(REACH + 128 * b, 128), :] = jnp.where(same, 1.0, 0.0).astype(BF)
            qext[pl.ds(128 * b, 128), :] = jnp.where(same, 0.0, -BIG).astype(BF)

    def build_halo_docs():
        void = jnp.where(sp == 0, 1.0, 0.0).astype(F32)
        for b in range(REACH // 128):
            r = (rows - REACH) // 128 + b
            col = doc_columns(halo_docs[r : r + 1, :])
            one_hot = jnp.where(col == lane_f, 1.0, 0.0)
            kext[pl.ds(128 * b, 128), :] = jnp.where(lane == 127, void, one_hot).astype(BF)

    def build_bias(layer):
        row = lax.broadcasted_iota(jnp.int32, (PAIR, PAIR), 0)
        col = lax.broadcasted_iota(jnp.int32, (PAIR, PAIR), 1)
        for n in range(2):
            near = table[layer, n : n + 1, 0 : 2 * MAX_REL]
            edge = table[layer, n : n + 1, 2 * MAX_REL : 2 * MAX_REL + 1]
            near = (near - edge) * LOG2E
            upper = jnp.concatenate([near[:, 128:], jnp.zeros((1, 128), F32)], axis=1)
            for part, values in ((0, upper), (1, near)):
                turned = pltpu.roll(
                    jnp.broadcast_to(values, (128, 256)), 128, 1, stride=1, stride_axis=0
                )[:, :128]
                if part == 1:
                    turned = jnp.where((row >= SEG) & (col < SEG), -BIG, turned)
                bias[layer, pl.ds(128 * part, 128), pl.ds(128 * n, 128)] = turned

    def project_qkv(layer, c, square_sum):
        scale = lax.rsqrt(square_sum * (1.0 / width) + 1e-06)
        qkv = jnp.dot(lhs[...], wqkv[layer], preferred_element_type=F32)
        q = qkv[:, 0:128] * (scale * (HEAD_DIM**-0.5 * LOG2E))
        k = qkv[:, 128:256] * scale
        v = qkv[:, 256:384] * scale
        wide = lax.broadcasted_iota(jnp.int32, (CHUNK, 128), 1)
        qbuf[0, chunk_rows(c), :] = jnp.where(wide < HEAD_DIM, q, 0.0).astype(BF)
        qbuf[1, chunk_rows(c), :] = jnp.where(wide < HEAD_DIM, 0.0, q).astype(BF)
        kbuf[layer, pl.ds(REACH + CHUNK * c, CHUNK), :] = k.astype(BF)
        for i in range(2):
            block = v[128 * i : 128 * (i + 1), :].T
            vt[layer, REACH // 128 + 2 * c + i] = block.astype(BF)

    def gain_row(layer, n, step):
        return gains[layer : layer + 1, pl.ds(n * step, step)].astype(F32)

    @scoped
    def dense(c):
        step = 256
        total = jnp.zeros((CHUNK, 128), F32)
        for n in range(width // step):
            x = h[chunk_rows(c), pl.ds(n * step, step)].astype(F32)
            square = x * x
            for j in range(step // 128):
                total = total + square[:, 128 * j : 128 * (j + 1)]
            lhs[:, pl.ds(n * step, step)] = (x * gain_row(0, n, step)).astype(BF)
        project_qkv(0, c, jnp.sum(total, axis=1, keepdims=True))

    @scoped
    def trans(c, between=None):
        step = 256
        a = jnp.concatenate([att[0, t, chunk_rows(c), :] for t in range(tp_n)], axis=1)
        total = jnp.zeros((CHUNK, 128), F32)
        for n in range(width // step):
            part = pl.ds(n * step, step)
            update = jnp.dot(a, wfirst[:, part], preferred_element_type=F32)
            x = (h[chunk_rows(c), part].astype(F32) + update).astype(BF)
            h[chunk_rows(c), part] = x
            x = x.astype(F32)
            square = x * x
            for j in range(step // 128):
                total = total + square[:, 128 * j : 128 * (j + 1)]
            lhs[:, part] = (x * gain_row(1, n, step)).astype(BF)
            if between is not None and n == width // step // 2 - 1:
                between()
        project_qkv(1, c, jnp.sum(total, axis=1, keepdims=True))

    @scoped
    def final(c, count=1):
        mine = pl.ds(c * CHUNK, count * CHUNK)
        a = jnp.concatenate([att[1, t, mine, :] for t in range(tp_n)], axis=1)
        update = jnp.dot(a, wlast[...], preferred_element_type=F32)
        own = h[mine, pl.ds(pl.multiple_of(me * cols, cols), cols)].astype(F32)
        mixed[mine, :] = (own + update).astype(BF)

    def scores_of(layer, p):
        window = pl.ds(PAIR * p, WIN)
        mine = pl.ds(PAIR * p, PAIR)
        keys = jnp.concatenate([kbuf[layer, window, :], kext[window, :]], axis=1)
        queries = jnp.concatenate(
            [
                jnp.concatenate([qbuf[0, mine, :], qext[mine, :]], axis=1),
                jnp.concatenate([qbuf[1, mine, :], qext[mine, :]], axis=1),
            ],
            axis=0,
        )
        s = lax.dot_general(
            keys, queries, (((1,), (1,)), ((), ())), preferred_element_type=F32
        )
        first = lax.broadcasted_iota(jnp.int32, (SEG, 2 * PAIR), 1)
        s_first = jnp.where(lax.rem(first, PAIR) < SEG, s[:SEG], -BIG)
        return jnp.concatenate(
            [s_first, s[SEG : WIN - 256], s[WIN - 256 :] + bias[layer]], axis=0
        )

    def weigh(layer, p, s):
        e = jnp.exp2(s - jnp.max(s, axis=0, keepdims=True))
        inverse = 1.0 / jnp.sum(e, axis=0, keepdims=True)
        values = jnp.concatenate([vt[layer, p + i] for i in range(WIN // 128)], axis=1)
        o = jnp.dot(values, e.astype(BF), preferred_element_type=F32)
        o = jnp.concatenate(
            [
                o[:HEAD_DIM, :PAIR] * inverse[:, :PAIR],
                o[HEAD_DIM:, PAIR:] * inverse[:, PAIR:],
            ],
            axis=0,
        )
        att[layer, me, pl.ds(PAIR * p, PAIR), :] = o.T.astype(BF)

    @scoped
    def attend(layer, *which):
        scores = [scores_of(layer, p) for p in which]
        for p, s in zip(which, scores):
            weigh(layer, p, s)

    def remote(src, dst, send_sem, recv_sem, device):
        return pltpu.make_async_remote_copy(
            src_ref=src,
            dst_ref=dst,
            send_sem=send_sem,
            recv_sem=recv_sem,
            device_id=device,
            device_id_type=MESH,
        )

    def halo(layer, c):
        i = layer * tail + c - (chunks - tail)
        k0 = CHUNK * (c - (chunks - tail))
        b0 = k0 // 128
        return (
            remote(
                kbuf.at[layer, pl.ds(REACH + CHUNK * c, CHUNK)],
                kbuf.at[layer, pl.ds(k0, CHUNK)],
                halo_send.at[2 * i],
                halo_recv.at[2 * i],
                succ,
            ),
            remote(
                vt.at[layer, pl.ds(REACH // 128 + 2 * c, 2)],
                vt.at[layer, pl.ds(b0, 2)],
                halo_send.at[2 * i + 1],
                halo_recv.at[2 * i + 1],
                succ,
            ),
        )

    def doc_halo():
        i = 2 * LAYERS * tail
        return remote(docs, halo_docs, halo_send.at[i], halo_recv.at[i], succ)

    halos = []

    def send_halo(layer, c):
        halos.extend(halo(layer, c))

        @pl.when(sp < sp_n - 1)
        def _():
            for copy in halo(layer, c):
                copy.start()

    @scoped
    def wait_halo(layer, c):
        @pl.when(sp > 0)
        def _():
            for copy in halo(layer, c):
                copy.wait_recv()

    sent = [0] * LAYERS

    def send(layer, c, slot, device, recv_sem, part=None):
        first = CHUNK * c + (PAIR if part == 1 else 0)
        count = CHUNK if part is None else PAIR
        ref = att.at[layer, slot, pl.ds(first, count)]
        remote(ref, ref, ag_send.at[layer], recv_sem, device).start()
        sent[layer] += count

    def arrived(layer, slots, recv_sem):
        ref = att.at[layer, 0:slots, pl.ds(0, CHUNK)]
        remote(ref, ref, ag_send.at[layer], recv_sem, partner).wait_recv()

    def near_sem(layer, c):
        return near_recv.at[layer * chunks + c]

    def far_sem(layer, c):
        return far_recv.at[layer * chunks + c]

    def partner_sem(layer, c):
        return partner_recv.at[layer * chunks + c]

    def is_direct(layer, c):
        return layer == 0 or c in DIRECT

    def send_own(layer, c):
        if is_direct(layer, c):
            send(layer, c, me, far, far_sem(layer, c))
        send(layer, c, me, right, near_sem(layer, c))
        send(layer, c, me, left, near_sem(layer, c))
        send(layer, c, me, partner, partner_sem(layer, c))

    @scoped
    def near(layer, c):
        arrived(layer, 2, near_sem(layer, c))
        if not is_direct(layer, c):
            send(layer, c, left_i, right, far_sem(layer, c), 0)
            send(layer, c, right_i, left, far_sem(layer, c), 1)
        send(layer, c, left_i, partner, partner_sem(layer, c))
        send(layer, c, right_i, partner, partner_sem(layer, c))

    @scoped
    def distant(layer, c):
        arrived(layer, 1, far_sem(layer, c))
        send(layer, c, far_i, partner, partner_sem(layer, c))

    @scoped
    def consume(layer, c):
        arrived(layer, tp_n // 2, partner_sem(layer, c))

    def attend_send(layer, c):
        attend(layer, 2 * c + 1, 2 * c)
        send_own(layer, c)

    @pl.when(sp == 0)
    def _():
        for layer in range(LAYERS):
            kbuf[layer, 0:REACH, :] = jnp.zeros((REACH, 128), BF)
            for b in range(REACH // 128):
                vt[layer, b] = jnp.zeros((128, 128), BF)
        halo_docs[...] = jnp.zeros(halo_docs.shape, jnp.int32)

    loads["docs"].wait()
    build_docs()
    loads["table"].wait()
    build_bias(0)
    for c in order[2:]:
        load_tokens(c)
    loads["gains"].wait()
    loads[("w", 0)].wait()
    c3, c2, c1, c0 = order
    loads[("t", c3)].wait()
    dense(c3)
    load("first", (out_first, wfirst))
    load_w(1)
    load("last", (out_last, wlast))
    loads[("t", c2)].wait()
    dense(c2)
    with jax.named_scope("barrier"):
        pl.semaphore_wait(barrier, 4 + jnp.where(sp > 0, 1, 0) + jnp.where(sp < sp_n - 1, 1, 0))
    send_halo(0, c3)

    @pl.when(sp < sp_n - 1)
    def _():
        doc_halo().start()

    send_halo(0, c2)
    loads[("t", c1)].wait()
    dense(c1)
    attend_send(0, c3)
    loads[("t", c0)].wait()
    dense(c0)
    attend_send(0, c2)

    @pl.when(sp > 0)
    def _():
        doc_halo().wait_recv()

    build_halo_docs()
    wait_halo(0, c3)
    attend(0, 3, 2)
    near(0, c3)
    distant(0, c3)
    send_own(0, c1)
    build_bias(1)
    loads["first"].wait()
    loads[("w", 1)].wait()
    loads["last"].wait()
    wait_halo(0, c2)
    attend_send(0, c0)
    consume(0, c3)

    def serve(c):
        near(0, c)
        distant(0, c)

    trans(c3, between=functools.partial(serve, c2))
    send_halo(1, c3)
    consume(0, c2)
    trans(c2, between=functools.partial(serve, c1))
    send_halo(1, c2)
    consume(0, c1)
    trans(c1)
    serve(c0)
    attend_send(1, c3)
    consume(0, c0)
    trans(c0)
    attend_send(1, c2)
    wait_halo(1, c3)
    attend_send(1, c1)
    wait_halo(1, c2)
    attend_send(1, c0)
    near(1, c3)
    distant(1, c3)
    near(1, c2)
    near(1, c1)
    consume(1, c3)
    final(c3)
    near(1, c0)
    distant(1, c0)
    consume(1, c0)
    final(c0)
    distant(1, c2)
    distant(1, c1)
    consume(1, c2)
    consume(1, c1)
    final(c1, 2)
    with jax.named_scope("sends"):
        for layer in range(LAYERS):
            whole, rest = divmod(sent[layer], rows)
            ref = att.at[layer, 0:whole]
            remote(ref, ref, ag_send.at[layer], near_sem(layer, 0), partner).wait_send()
            if rest:
                ref = att.at[layer, 0, pl.ds(0, rest)]
                remote(ref, ref, ag_send.at[layer], near_sem(layer, 0), partner).wait_send()

        @pl.when(sp < sp_n - 1)
        def _():
            doc_halo().wait_send()
            for copy in halos:
                copy.wait_send()


def solution(mesh):
    sp_n, tp_n = mesh.shape["sp"], mesh.shape["tp"]

    def shards(tokens, doc_ids, gains, w_query, w_key, w_value, rel_table, out_first, out_last):
        rows, width = tokens.shape
        cols = out_last.shape[1]
        depth = out_first.shape[0]
        heads = w_query.shape[2]
        tail = REACH // CHUNK
        halos = 2 * LAYERS * tail + 1
        anywhere = pl.BlockSpec(memory_space=pltpu.HBM)
        vmem = pl.BlockSpec(memory_space=pltpu.VMEM)
        return pl.pallas_call(
            functools.partial(kernel, sp_n, tp_n),
            out_shape=jax.ShapeDtypeStruct((rows, cols), BF),
            in_specs=[anywhere] * 9,
            out_specs=vmem,
            scratch_shapes=[
                pltpu.VMEM((rows // 128, 128), jnp.int32),
                pltpu.VMEM(gains.shape, gains.dtype),
                pltpu.VMEM(rel_table.shape, rel_table.dtype),
                pltpu.VMEM((rows, width), BF),
                pltpu.VMEM((CHUNK, width), BF),
                pltpu.VMEM((LAYERS, width, 3 * heads), BF),
                pltpu.VMEM((depth, width), BF),
                pltpu.VMEM((depth, cols), BF),
                pltpu.VMEM((2, rows, heads), BF),
                pltpu.VMEM((rows, 128), BF),
                pltpu.VMEM((LAYERS, REACH + rows, heads), BF),
                pltpu.VMEM((REACH + rows, 128), BF),
                pltpu.VMEM((LAYERS, (REACH + rows) // 128, heads, 128), BF),
                pltpu.VMEM((LAYERS, tp_n, rows, heads), BF),
                pltpu.VMEM((LAYERS, 256, 2 * PAIR), F32),
                pltpu.VMEM((rows // 128, 128), jnp.int32),
                pltpu.SemaphoreType.DMA((LAYERS + rows // CHUNK + 5,)),
                pltpu.SemaphoreType.DMA((halos,)),
                pltpu.SemaphoreType.DMA((halos,)),
                pltpu.SemaphoreType.DMA((LAYERS,)),
                pltpu.SemaphoreType.DMA((LAYERS * (rows // CHUNK),)),
                pltpu.SemaphoreType.DMA((LAYERS * (rows // CHUNK),)),
                pltpu.SemaphoreType.DMA((LAYERS * (rows // CHUNK),)),
            ],
            compiler_params=pltpu.CompilerParams(
                collective_id=0, has_side_effects=True, vmem_limit_bytes=40 * 1024 * 1024
            ),
        )(
            *[
                pltpu.with_memory_space_constraint(x, pltpu.HBM)
                for x in (
                    tokens,
                    doc_ids.reshape(rows // 128, 128),
                    gains,
                    w_query,
                    w_key,
                    w_value,
                    rel_table,
                    out_first,
                    out_last,
                )
            ],
        )

    placed = (
        P(("grp", "sp"), None),
        P(("grp", "sp")),
        P(),
        P(None, None, "tp"),
        P(None, None, "tp"),
        P(None, None, "tp"),
        P(None, "tp", None),
        P(),
        P(None, "tp"),
    )
    return jax.shard_map(
        shards, mesh=mesh, in_specs=placed, out_specs=P(("grp", "sp"), "tp"), check_vma=False
    )
```
